32 devices in a mesh: ep: 8 (over z, y), tp: 4 (over x, core).
Axes of the slice: x: 2, y: 2, z: 4, core: 2. Of those that a mesh axis runs over, the one named last changes fastest.
Arguments:
- conv_value: bfloat16 [4096, 2048], P('ep', 'tp'), may hold values from -6 to 6
- conv_gate: bfloat16 [4096, 2048], P('ep', 'tp'), may hold values from -9 to 9
- conv_kernel: float32 [31, 2048], P(None, 'tp'), may hold values from -20 to 20
- norm_gain: float32 [2048], P('tp'), may hold values from 0.1 to 1.9
- mixer_proj: bfloat16 [2048, 2048], P('tp'), may hold values from -0.125 to 0.125
- moe_in: bfloat16 [4096, 2048], P('ep'), may hold values from -6 to 6
- route_ids: int32 [4096, 2], P('ep'), may hold values from 0 to 7, all different within a row; in each aligned block of 128 rows (0 to 127, 128 to 255, ...) at most 64 rows name the same one
- route_logits: float32 [4096, 2], P('ep'), may hold values from -6 to 6
- moe_gain: float32 [2048], replicated, may hold values from 0.1 to 1.9
- expert_gate: bfloat16 [8, 2048, 2048], P('ep', None, 'tp'), may hold values from -0.26367188 to 0.26367188
- expert_lin: bfloat16 [8, 2048, 2048], P('ep', None, 'tp'), may hold values from -0.26367188 to 0.26367188
- expert_down: bfloat16 [8, 2048, 2048], P('ep', 'tp'), may hold values from -0.052978516 to 0.052978516
Outputs:
- mixer_out: bfloat16 [4096, 2048], P(('ep', 'tp'))
- moe_out: bfloat16 [4096, 2048], P(('ep', 'tp'))
The draws below stay inside these ranges and needn't reach their ends.
Inputs may be any that keep to these rules, and one draw needn't show every extreme that they name: `route_ids`: every row names 2 different experts. In each aligned block of 128 rows (one device's output rows) no expert is named by more than 64 rows, and in every draw some expert is named by exactly 64 rows of some block.
All inputs are finite; a program needn't handle non-finite values.
Results may differ from the reference program's by a relative error of at most 0.01.
Values may be sent and summed in bfloat16 or wider, within the bound.
No kernel may reach another device: no remote copies, remote signals or barrier semaphores. Data moves between devices by JAX's collectives and lax.ppermute only.
A program may use at most 128 MiB of HBM per device.

```python
import math
import jax
import jax.numpy as jnp
import numpy as np
from jax import lax

D = 2048
C = 2048
F = 2048
KW = 31
TOPK = 2
ROWS = 128
EXPERTS = 8
CAP = 64
TOKM = 4096
TOKE = 4096
N_TP = 4


def draw_conv_kernel(key, part):
    first = jax.random.fold_in(key, 11)
    second = jax.random.fold_in(key, 12)
    base = jax.random.normal(first, (KW, C), jnp.float32)
    spread = jnp.exp(jax.random.uniform(second, (1, C), jnp.float32, -0.5, 0.5))
    rising = jnp.exp(math.log(10.0) * jnp.arange(C, dtype=jnp.float32) / C)[None, :]
    return base * spread * rising / math.sqrt(KW)


def levels(key, shape, pieces, low, top_value):
    factor_of, own = 1.0, jax.random.fold_in(key, 6)
    for position, shards_of in pieces:
        steps = jnp.exp(jax.random.uniform(jax.random.fold_in(own, position), (shards_of,), jnp.float32, low / len(pieces), top_value / len(pieces)))
        factor_of = factor_of * jnp.repeat(steps, shape[position] // shards_of).reshape([-1 if axis == position else 1 for axis in range(len(shape))])
    return factor_of


def routed_block(own_key, own, number, rows, count, top, bound, slope):
    order = jax.random.permutation(own_key, count)
    heavy_load, common = portions_of(count, rows * top, bound, slope, True), portions_of(count, rows * top, bound, slope, False)
    places = jnp.arange(count)

    def named(lengths, turn):
        used = int((lengths > 0).sum())
        fixed = max(1, used // 4)
        moved = fixed + (places - fixed + turn * (used - fixed)) % max(1, count - fixed)
        return jnp.zeros((count,), jnp.int32).at[order[jnp.where(places < fixed, places, moved)]].set(jnp.asarray(lengths, jnp.int32))

    lengths = jnp.where(number % 4 == 0, named(heavy_load, number // 4), named(common, number - number // 4 - 1))
    mixed = jax.random.permutation(jax.random.fold_in(own, 3), count)
    giver, sink = mixed[0:count // 2 * 2:2], mixed[1:count // 2 * 2:2]
    slack = jnp.minimum(lengths[giver] - 1, bound - lengths[sink]) // 2
    slack = jnp.where((giver == order[0]) | (sink == order[0]) | (lengths[sink] == 0), 0, jnp.maximum(slack, 0))
    moved = jax.random.randint(jax.random.fold_in(own, 4), (count // 2,), 0, 1 << 20) % (slack + 1)
    lengths = lengths.at[giver].add(-moved).at[sink].add(moved)
    items = jnp.searchsorted(jnp.cumsum(lengths), jnp.arange(rows * top), side="right").astype(jnp.int32)
    table = items.reshape(top, rows).T
    table = table[jax.random.permutation(jax.random.fold_in(own, 1), rows)]
    turn = jax.random.randint(jax.random.fold_in(own, 2), (rows, 1), 0, top)
    return jnp.take_along_axis(table, (jnp.arange(top)[None, :] + turn) % top, axis=1)


def portions_of(number_of, total, reach, skew, full):
    portions = [(1 << 20) // math.isqrt(standing ** skew) + 1 for standing in range(1, number_of + 1)]
    largest = reach if full else min(reach, max(-(-total // number_of), total * portions[0] // sum(portions)))
    least = 1 if total - largest >= number_of - 1 else 0
    given, surplus = [largest] + [least] * (number_of - 1), total - largest - least * (number_of - 1)
    while surplus > 0:
        candidates = [i for i in range(1, number_of) if given[i] < largest] or [i for i in range(1, number_of) if given[i] < reach]
        whole, remaining = sum([portions[i] for i in candidates]), surplus
        for i in candidates:
            more = min(reach - given[i], max(1, remaining * portions[i] // whole), surplus)
            given[i] = given[i] + more
            surplus = surplus - more
    return np.array(given)


def gaussian(rng, shape, width, limit, shards=(), kind=jnp.bfloat16):
    result = jax.random.normal(rng, shape, jnp.float32) * width
    if len(shards) > 0:
        result = levels(rng, shape, shards, -0.22, 0.18) * result
    return jnp.clip(result, min=-limit, max=limit).astype(kind)


def setup_inputs(seed: int = 0) -> dict:
    keys = jax.random.split(jax.random.key(seed), 13)
    conv_value = gaussian(keys[0], (TOKM, C), 1.0, 6.0, ((0, 8), (1, 4)))
    conv_gate = gaussian(keys[1], (TOKM, C), 1.5, 9.0, ((0, 8), (1, 4)))
    conv_kernel = draw_conv_kernel(jax.random.fold_in(keys[12], 71), 0)
    norm_gain = jnp.clip(1.0 + 0.18 * jax.random.normal(keys[3], (C,), jnp.float32), 0.1, 1.9)
    mixer_proj = gaussian(keys[4], (C, D), C ** -0.5, 0.125, ((0, 4),))
    moe_in = gaussian(keys[5], (TOKE, D), 1.0, 6.0, ((0, 8),))
    route_ids_keys = jax.random.split(jax.random.fold_in(keys[6], 1), TOKE // ROWS)
    route_ids_turns = jax.random.permutation(jax.random.fold_in(keys[6], 3), TOKE // ROWS)
    route_ids = jax.vmap(lambda own, number: routed_block(jax.random.fold_in(keys[6], 2), own, number, ROWS, EXPERTS, TOPK, CAP, 1))(route_ids_keys, route_ids_turns).reshape((TOKE, TOPK))
    route_logits = gaussian(keys[7], (TOKE, TOPK), 1.5, 6.0, ((0, 8),), jnp.float32)
    moe_gain = jnp.clip(1.0 + 0.18 * jax.random.normal(keys[8], (D,), jnp.float32), 0.1, 1.9)
    expert_gate = gaussian(keys[9], (EXPERTS, D, F), (2.0 * D ** -0.5), 0.26367188, ((0, 8), (2, 4)))
    expert_lin = gaussian(keys[10], (EXPERTS, D, F), (2.0 * D ** -0.5), 0.26367188, ((0, 8), (2, 4)))
    expert_down = gaussian(keys[11], (EXPERTS, F, D), (0.4 * F ** -0.5), 0.052978516, ((0, 8), (1, 4)))
    return {"conv_value": conv_value, "conv_gate": conv_gate, "conv_kernel": conv_kernel, "norm_gain": norm_gain, "mixer_proj": mixer_proj, "moe_in": moe_in, "route_ids": route_ids, "route_logits": route_logits, "moe_gain": moe_gain, "expert_gate": expert_gate, "expert_lin": expert_lin, "expert_down": expert_down}


EPS = 1e-05
LIMIT = 7.0
SLOPE = 1.702

def slot_targets(routes, experts, capacity):
    flat = routes.reshape(-1)
    onehot = (flat[:, None] == jnp.arange(experts, dtype=jnp.int32)[None, :]).astype(jnp.int32)
    rank = lax.optimization_barrier(jnp.sum(jnp.cumsum(onehot, axis=0) * onehot, axis=1)) - 1
    return (flat * capacity + rank).astype(jnp.int32)

def slot_sources(target, total, topk):
    hits = (target[None, :] == jnp.arange(total, dtype=jnp.int32)[:, None]).astype(jnp.int32)
    owner = jnp.arange(target.shape[0], dtype=jnp.int32) // topk
    source = lax.optimization_barrier(jnp.sum(hits * owner[None, :], axis=1)).astype(jnp.int32)
    filled = lax.optimization_barrier(jnp.sum(hits, axis=1)) > 0
    return (source, filled)

def reference(conv_value, conv_gate, conv_kernel, norm_gain, mixer_proj, moe_in, route_ids, route_logits, moe_gain, expert_gate, expert_lin, expert_down):
    glu = (conv_value.astype(jnp.float32) * jax.nn.sigmoid(conv_gate.astype(jnp.float32))).astype(jnp.bfloat16)
    padded = jnp.pad(glu.astype(jnp.float32), ((KW - 1, 0), (0, 0)))
    conv = jnp.zeros((TOKM, C), jnp.float32)
    for tap in range(KW):
        conv = conv + conv_kernel[tap][None, :] * padded[tap:tap + TOKM]
    mean = lax.optimization_barrier(jnp.mean(conv, axis=1, keepdims=True))
    var = lax.optimization_barrier(jnp.mean(jnp.square(conv - mean), axis=1, keepdims=True))
    conv_act = jax.nn.silu((conv - mean) * lax.rsqrt(var + EPS) * norm_gain).astype(jnp.bfloat16)
    block_c = C // N_TP
    mixer_sum = jnp.zeros((TOKM, D), jnp.float32)
    for part in range(N_TP):
        term = jnp.dot(conv_act[:, part * block_c:(part + 1) * block_c], mixer_proj[part * block_c:(part + 1) * block_c], preferred_element_type=jnp.float32)
        mixer_sum = mixer_sum + term.astype(jnp.bfloat16).astype(jnp.float32)
    mixer_out = mixer_sum.astype(jnp.bfloat16)
    xin = moe_in.astype(jnp.float32)
    mu = lax.optimization_barrier(jnp.mean(xin, axis=1, keepdims=True))
    va = lax.optimization_barrier(jnp.mean(jnp.square(xin - mu), axis=1, keepdims=True))
    moe_norm = ((xin - mu) * lax.rsqrt(va + EPS) * moe_gain).astype(jnp.bfloat16)
    blocks = TOKE // ROWS
    routes = route_ids.reshape(blocks, ROWS, TOPK)
    targets = jax.vmap(lambda r: slot_targets(r, EXPERTS, CAP))(routes)
    sources, filled = jax.vmap(lambda t: slot_sources(t, EXPERTS * CAP, TOPK))(targets)
    base = (jnp.arange(blocks, dtype=jnp.int32) * ROWS)[:, None]
    global_src = (sources + base).reshape(blocks, EXPERTS, CAP)
    live = filled.reshape(blocks, EXPERTS, CAP)
    block_f = F // N_TP

    def one_expert(expert):
        index = lax.dynamic_index_in_dim(global_src, expert, 1, keepdims=False).reshape(-1)
        mask = lax.dynamic_index_in_dim(live, expert, 1, keepdims=False).reshape(-1)
        rows = jnp.where(mask[:, None], moe_norm[index], jnp.zeros((), jnp.bfloat16))
        gate = jnp.minimum(jnp.dot(rows, expert_gate[expert], preferred_element_type=jnp.float32), LIMIT)
        lin = jnp.clip(jnp.dot(rows, expert_lin[expert], preferred_element_type=jnp.float32), -LIMIT, LIMIT)
        hidden = (gate * jax.nn.sigmoid(SLOPE * gate) * (lin + 1.0)).astype(jnp.bfloat16)
        down = expert_down[expert]
        total = jnp.zeros((rows.shape[0], D), jnp.float32)
        for part in range(N_TP):
            term = jnp.dot(hidden[:, part * block_f:(part + 1) * block_f], down[part * block_f:(part + 1) * block_f], preferred_element_type=jnp.float32)
            total = total + term.astype(jnp.bfloat16).astype(jnp.float32)
        return total.astype(jnp.bfloat16)
    outputs = lax.map(one_expert, jnp.arange(EXPERTS, dtype=jnp.int32))
    flat_out = outputs.reshape(EXPERTS * blocks * CAP, D)
    expert_id = targets // CAP
    slot = targets % CAP
    where = (expert_id * (blocks * CAP) + jnp.arange(blocks, dtype=jnp.int32)[:, None] * CAP + slot).reshape(-1)
    picked = flat_out[where].astype(jnp.float32).reshape(TOKE, TOPK, D)
    expo = jnp.exp(route_logits)
    weight = expo / lax.optimization_barrier(jnp.sum(expo, axis=1, keepdims=True))
    moe_out = lax.optimization_barrier(jnp.sum(picked * weight[:, :, None], axis=1)).astype(jnp.bfloat16)
    return (mixer_out, moe_out)
```

```python
import jax
import jax.numpy as jnp
from jax import lax
from jax.sharding import PartitionSpec as P

EPS = 1e-05
LIMIT = 7.0
SLOPE = 1.702
BF16 = jnp.bfloat16
F32 = jnp.float32


def dot(a, b):
    return jnp.dot(a, b, preferred_element_type=F32)


def tp_swap(block, bit):
    return lax.ppermute(block, "tp", [(i, i ^ bit) for i in range(lax.axis_size("tp"))])


def ep_route(size, k, dy):
    half = size // 2
    return [(e, ((e // 2 + k) % half) * 2 + ((e % 2) ^ dy)) for e in range(size)]


def ep_send(block, k, dy):
    return lax.ppermute(block, "ep", ep_route(lax.axis_size("ep"), k, dy))


def ep_return(block, k, dy):
    route = [(b, a) for a, b in ep_route(lax.axis_size("ep"), k, dy)]
    return lax.ppermute(block, "ep", route)


def passed_along(block, axis, distance):
    devices = range(lax.axis_size(axis))
    route = [(i - distance, i) for i in devices if i - distance in devices]
    return lax.ppermute(block, axis, route)


def norm_rows(block, gain):
    block = block.astype(F32)
    mu = jnp.mean(block, axis=1, keepdims=True)
    va = jnp.mean(jnp.square(block - mu), axis=1, keepdims=True)
    return ((block - mu) * lax.rsqrt(va + EPS) * gain).astype(BF16)


def slot_table(places, experts, capacity):
    rows, topk = places.shape
    flat = places.reshape(-1)
    onehot = flat[:, None] == jnp.arange(experts, dtype=jnp.int32)[None, :]
    count = flat.shape[0]
    step = jnp.arange(count, dtype=jnp.int32)
    before = (step[None, :] < step[:, None]).astype(BF16)
    ahead = dot(before, onehot.astype(BF16))
    rank = jnp.sum(jnp.where(onehot, ahead, 0.0), axis=1).astype(jnp.int32)
    return (flat * capacity + rank).reshape(rows, topk)


def packed_rows(slots, normed, total):
    number = jnp.arange(total, dtype=jnp.int32)[:, None]
    hit = slots[:, 0][None, :] == number
    for j in range(1, slots.shape[1]):
        hit = hit | (slots[:, j][None, :] == number)
    return dot(hit.astype(BF16), normed).astype(BF16)


def expert_rows(rows, gates, lins, downs):
    total = None
    for wg, wl, wd in zip(gates, lins, downs, strict=True):
        gate = jnp.minimum(dot(rows, wg), LIMIT)
        lin = jnp.clip(dot(rows, wl), -LIMIT, LIMIT)
        hidden = (gate * jax.nn.sigmoid(SLOPE * gate) * (lin + 1.0)).astype(BF16)
        part = dot(hidden, wd)
        total = part if total is None else total + part
    return total.astype(BF16)


def mixer(conv_value, conv_gate, conv_kernel, norm_gain, mixer_proj):
    core = lax.axis_index("tp") % 2
    x = lax.axis_index("tp") // 2
    glu = (conv_value.astype(F32) * jax.nn.sigmoid(conv_gate.astype(F32))).astype(BF16)
    reach = conv_kernel.shape[0] - 1
    length = glu.shape[0]
    rim = passed_along(glu[length - reach :], "ep", 1)
    padded = jnp.concatenate([rim, glu], axis=0).astype(F32)
    conv = jnp.zeros(glu.shape, F32)
    for tap in range(reach + 1):
        conv = conv + conv_kernel[tap][None, :] * padded[tap : tap + length]
    sums = jnp.stack([jnp.sum(conv, axis=1), jnp.sum(conv * conv, axis=1)])
    sums = sums + tp_swap(sums, 1)
    sums = sums + tp_swap(sums, 2)
    channels = conv.shape[1] * lax.axis_size("tp")
    mean = (sums[0] / channels)[:, None]
    var = (sums[1] / channels)[:, None] - mean * mean
    act = jax.nn.silu((conv - mean) * lax.rsqrt(var + EPS) * norm_gain).astype(BF16)
    rows = length // 4
    act = act.reshape(2, 2, rows, -1)
    mine = jnp.where(core == 0, act[:, 0], act[:, 1])
    other = tp_swap(jnp.where(core == 0, act[:, 1], act[:, 0]), 1)
    proj_other = tp_swap(mixer_proj, 1)
    flat = lambda a: a.reshape(2 * rows, -1)
    part = dot(flat(mine), mixer_proj) + dot(flat(other), proj_other)
    part = part.reshape(2, rows, -1).astype(BF16)
    away = tp_swap(jnp.where(x == 0, part[1], part[0]), 2)
    kept = jnp.where(x == 0, part[0], part[1])
    return (kept.astype(F32) + away.astype(F32)).astype(BF16)


def experts_layer(moe_in, route_ids, route_logits, moe_gain, expert_gate, expert_lin, expert_down):
    tp_size = lax.axis_size("tp")
    experts = lax.axis_size("ep")
    half = experts // 2
    me = lax.axis_index("ep")
    t = lax.axis_index("tp")
    rows = moe_in.shape[0] // tp_size
    topk = route_ids.shape[1]
    capacity = max(2, 2 * rows * topk // experts)

    def own(a, index):
        return lax.dynamic_slice_in_dim(a, index * rows, rows, 0)

    def place(ids):
        return ((ids // 2 - me // 2) % half) * 2 + (ids + me) % 2

    slots = slot_table(place(own(route_ids, t)), experts, capacity)
    slots_x = slot_table(place(own(route_ids, t ^ 2)), experts, capacity)
    pack = packed_rows(slots, norm_rows(own(moe_in, t), moe_gain), experts * capacity)
    pack_x = packed_rows(slots_x, norm_rows(own(moe_in, t ^ 2), moe_gain), 2 * capacity)

    def message(a, place_number):
        return a[place_number * capacity : (place_number + 1) * capacity]

    gates = (expert_gate[0], tp_swap(expert_gate[0], 1))
    lins = (expert_lin[0], tp_swap(expert_lin[0], 1))
    downs = (expert_down[0], tp_swap(expert_down[0], 1))
    near = ep_send(jnp.concatenate([message(pack, 1), message(pack_x, 1)], axis=0), 0, 1)
    order = [1] + list(range(3, half)) + [2] if half > 2 else list(range(1, half))
    landed = {}
    for k in order:
        landed[k] = jnp.concatenate([ep_send(message(pack, 2 * k + dy), k, dy) for dy in range(2)], axis=0)
    chunk = {
        0: jnp.concatenate(
            [message(pack, 0), message(near, 0), message(pack_x, 0), message(near, 1)], axis=0
        )
    }
    for k in order:
        chunk[k] = jnp.concatenate([landed[k], tp_swap(landed[k], 2)], axis=0)
    back = {}
    for k in order + [0]:
        part = expert_rows(chunk[k], gates, lins, downs)
        kept, sent = part[: 2 * capacity], part[2 * capacity :]
        out = (kept.astype(F32) + tp_swap(sent, 2).astype(F32)).astype(BF16)
        for dy in range(2):
            piece = message(out, dy)
            back[2 * k + dy] = piece if (k, dy) == (0, 0) else ep_return(piece, k, dy)
    returned = jnp.concatenate([back[i] for i in range(experts)], axis=0)
    expo = jnp.exp(own(route_logits, t))
    weight = expo / jnp.sum(expo, axis=1, keepdims=True)
    number = jnp.arange(experts * capacity, dtype=jnp.int32)[None, :]
    table = sum(
        jnp.where(slots[:, j][:, None] == number, weight[:, j][:, None], 0.0) for j in range(topk)
    )
    high = lax.reduce_precision(table, 8, 7)
    low = (table - high).astype(BF16)
    return (dot(high.astype(BF16), returned) + dot(low, returned)).astype(BF16)


def shards(
    conv_value,
    conv_gate,
    conv_kernel,
    norm_gain,
    mixer_proj,
    moe_in,
    route_ids,
    route_logits,
    moe_gain,
    expert_gate,
    expert_lin,
    expert_down,
):
    mixer_out = mixer(conv_value, conv_gate, conv_kernel, norm_gain, mixer_proj)
    moe_out = experts_layer(
        moe_in, route_ids, route_logits, moe_gain, expert_gate, expert_lin, expert_down
    )
    return (mixer_out, moe_out)


def solution(mesh):
    placed = (
        P("ep", "tp"),
        P("ep", "tp"),
        P(None, "tp"),
        P("tp"),
        P("tp", None),
        P("ep", None),
        P("ep", None),
        P("ep", None),
        P(),
        P("ep", None, "tp"),
        P("ep", None, "tp"),
        P("ep", "tp", None),
    )
    return jax.shard_map(
        shards,
        mesh=mesh,
        in_specs=placed,
        out_specs=(P(("ep", "tp"), None), P(("ep", "tp"), None)),
        check_vma=False,
    )
```

```python
import functools

import jax
import jax.numpy as jnp
from jax import lax
from jax.experimental import pallas as pl
from jax.experimental.pallas import tpu as pltpu
from jax.sharding import PartitionSpec as P

EPS = 1e-05
LIMIT = 7.0
SLOPE = 1.702
BF16 = jnp.bfloat16
F32 = jnp.float32

FEW = 8


def few_experts(experts):
    return experts <= FEW and experts & (experts - 1) == 0


def dot(a, b):
    return jnp.dot(a, b, preferred_element_type=F32)


def tp_swap(block, bit):
    return lax.ppermute(block, "tp", [(i, i ^ bit) for i in range(lax.axis_size("tp"))])


def ep_swap(block, place):
    size = lax.axis_size("ep")
    return lax.ppermute(block, "ep", [(e, e ^ place) for e in range(size)])


def passed_along(block, axis, distance):
    devices = range(lax.axis_size(axis))
    route = [(i - distance, i) for i in devices if i - distance in devices]
    return lax.ppermute(block, axis, route)


def pack_body(experts, capacity, layout, turn_ref, own_ref, far_ref, ids_ref, ids_far_ref, gain_ref, slots_ref, slots_far_ref, *outs):
    topk, rows = ids_ref.shape
    me = turn_ref[2]

    def placed(ids):
        return ids ^ me if layout["turned"] else ids

    def slots_of(ids):
        place = placed(ids)
        number = lax.broadcasted_iota(jnp.int32, (experts, rows), 0)
        named = [place[j : j + 1] == number for j in range(topk)]
        any_named = functools.reduce(jnp.logical_or, named).astype(F32).astype(BF16)
        row = lax.broadcasted_iota(jnp.int32, (rows, rows), 0)
        col = lax.broadcasted_iota(jnp.int32, (rows, rows), 1)
        ahead = dot(any_named, (row < col).astype(F32).astype(BF16))
        rank = [
            jnp.sum(jnp.where(hit, ahead, 0.0), axis=0, keepdims=True).astype(jnp.int32)
            for hit in named
        ]
        return [place[j : j + 1] * capacity + rank[j] for j in range(topk)]

    def normed(ref):
        block = ref[...].astype(F32)
        mu = jnp.mean(block, axis=1, keepdims=True)
        off = block - mu
        va = jnp.mean(off * off, axis=1, keepdims=True)
        return (off * lax.rsqrt(va + EPS) * gain_ref[...]).astype(BF16)

    def packed(slots, block, count):
        number = lax.broadcasted_iota(jnp.int32, (count * capacity, rows), 0)
        hit = functools.reduce(jnp.logical_or, [slot == number for slot in slots])
        return dot(hit.astype(F32).astype(BF16), block).astype(BF16)

    slots, slots_far = slots_of(ids_ref[...]), slots_of(ids_far_ref[...])
    for j in range(topk):
        slots_ref[j : j + 1] = slots[j]
        slots_far_ref[j : j + 1] = slots_far[j]
    whole = packed(slots, normed(own_ref), experts)
    far = packed(slots_far, normed(far_ref), layout["far"]) if layout["far"] else None
    for out, parts in zip(outs, layout["outs"], strict=True):
        at = 0
        for source, first, count in parts:
            size = count * capacity
            out[at : at + size] = (far if source else whole)[first * capacity : first * capacity + size]
            at += size


def pack_tokens(turn, moe_in, route_ids, gain, capacity, layout):
    tp_size = lax.axis_size("tp")
    experts = lax.axis_size("ep")
    rows, width = moe_in.shape[0] // tp_size, moe_in.shape[1]
    topk = route_ids.shape[1]
    sizes = [sum(part[2] for part in parts) * capacity for parts in layout["outs"]]
    fixed = lambda shape: pl.BlockSpec(shape, lambda i, s: (0, 0))
    return pl.pallas_call(
        functools.partial(pack_body, experts, capacity, layout),
        grid_spec=pltpu.PrefetchScalarGridSpec(
            num_scalar_prefetch=1,
            grid=(1,),
            in_specs=[
                pl.BlockSpec((rows, width), lambda i, s: (s[0], 0)),
                pl.BlockSpec((rows, width), lambda i, s: (s[1], 0)),
                pl.BlockSpec((topk, rows), lambda i, s: (0, s[0])),
                pl.BlockSpec((topk, rows), lambda i, s: (0, s[1])),
                fixed((1, width)),
            ],
            out_specs=[fixed((topk, rows))] * 2 + [fixed((size, width)) for size in sizes],
        ),
        out_shape=[jax.ShapeDtypeStruct((topk, rows), jnp.int32)] * 2
        + [jax.ShapeDtypeStruct((size, width), BF16) for size in sizes],
        compiler_params=pltpu.CompilerParams(vmem_limit_bytes=16 * 2**20),
        cost_estimate=pl.CostEstimate(flops=2**30, bytes_accessed=2**22, transcendentals=0),
    )(turn, moe_in, moe_in, route_ids.T, route_ids.T, gain[None, :])


def merge_body(parts, extra, t_ref, slots_ref, logits_ref, *refs):
    ins, out, held = refs[: len(parts)], refs[-2], refs[-1]
    at = 0
    for ref, (first, size) in zip(ins, parts, strict=True):
        held[at : at + size] = ref[first : first + size]
        at += size
    topk, rows = slots_ref.shape
    expo = jnp.exp(logits_ref[...])
    weight = expo / jnp.sum(expo, axis=0, keepdims=True)
    number = lax.broadcasted_iota(jnp.int32, (at, rows), 0)
    table = jnp.zeros((at, rows), F32)
    for j in range(topk):
        table = table + jnp.where(slots_ref[j : j + 1] == number, weight[j : j + 1], 0.0)
    high = table.astype(BF16)
    low = (table - high.astype(F32)).astype(BF16)
    both = jnp.concatenate([high, low], axis=1)
    both = lax.dot_general(both, held[...], (((0,), (0,)), ((), ())), preferred_element_type=F32)
    total = both[:rows] + both[rows:]
    if extra:
        total = total + refs[len(parts)][...].astype(F32)
    out[...] = total.astype(BF16)


def merge_rows(slots, route_logits, block, pieces, parts, extra=()):
    topk, rows = slots.shape
    width = pieces[0].shape[1]
    total = sum(size for _, size in parts)
    fixed = lambda shape: pl.BlockSpec(shape, lambda i, s: (0, 0))
    return pl.pallas_call(
        functools.partial(merge_body, parts, len(extra)),
        grid_spec=pltpu.PrefetchScalarGridSpec(
            num_scalar_prefetch=1,
            grid=(1,),
            in_specs=[fixed((topk, rows)), pl.BlockSpec((topk, rows), lambda i, s: (0, s[0]))]
            + [fixed(piece.shape) for piece in (*pieces, *extra)],
            out_specs=fixed((rows, width)),
            scratch_shapes=[pltpu.VMEM((total, width), BF16)],
        ),
        out_shape=jax.ShapeDtypeStruct((rows, width), BF16),
        compiler_params=pltpu.CompilerParams(vmem_limit_bytes=12 * 2**20),
        cost_estimate=pl.CostEstimate(flops=2**29, bytes_accessed=2**22, transcendentals=0),
    )(block, slots, route_logits.T, *pieces, *extra)


def ffn_body(pieces, targets, *refs):
    ins, refs = refs[:pieces], refs[pieces:]
    wg0, wg1, wl0, wl1, wd0, wd1 = refs[:6]
    givers = refs[6 : 6 + targets]
    rows, ups, downs, hidden, outs, sems = refs[6 + targets :]
    d, f = wg0.shape
    row_copies = []
    at = 0
    for ref in ins:
        row_copies.append((ref, rows.at[at : at + ref.shape[0]]))
        at += ref.shape[0]
    up_copies = [(ref, ups.at[i]) for i, ref in enumerate((wg0, wl0, wg1, wl1))]
    down_copies = [(ref, downs.at[i * f : (i + 1) * f]) for i, ref in enumerate((wd0, wd1))]
    copies = [
        pltpu.make_async_copy(source, target, sems.at[i])
        for i, (source, target) in enumerate(row_copies + up_copies + down_copies)
    ]
    r = len(row_copies)
    for copy in copies[: r + 4]:
        copy.start()
    for copy in copies[: r + 2]:
        copy.wait()
    for copy in copies[r + 4 :]:
        copy.start()
    t = min(256, f)
    for source in range(2):
        if source == 1:
            copies[r + 2].wait()
            copies[r + 3].wait()
        for at in range(0, f, t):
            gate = jnp.minimum(dot(rows[...], ups[2 * source, :, at : at + t]), LIMIT)
            lin = jnp.clip(dot(rows[...], ups[2 * source + 1, :, at : at + t]), -LIMIT, LIMIT)
            to = source * f + at
            hidden[:, to : to + t] = (gate * jax.nn.sigmoid(SLOPE * gate) * (lin + 1.0)).astype(BF16)
    copies[r + 4].wait()
    copies[r + 5].wait()
    t = min(512, d)
    last = []
    for at in range(0, d, t):
        outs[:, at : at + t] = dot(hidden[...], downs[:, at : at + t]).astype(BF16)
        first = 0
        for giver in givers:
            size = giver.shape[0]
            copy = pltpu.make_async_copy(
                outs.at[first : first + size, at : at + t],
                giver.at[:, at : at + t],
                sems.at[r + 6 + len(last)],
            )
            copy.start()
            last.append(copy)
            first += size
    for copy in last:
        copy.wait()


def expert_rows(pieces, gates, lins, downs):
    m = sum(piece.shape[0] for piece in pieces)
    d, f = gates[0].shape
    anywhere = pl.BlockSpec(memory_space=pl.ANY)
    copies = len(pieces) + 6 + len(pieces) * (d // min(512, d))
    return pl.pallas_call(
        functools.partial(ffn_body, len(pieces), len(pieces)),
        in_specs=[anywhere] * len(pieces) + [pl.BlockSpec(memory_space=pltpu.HBM)] * 6,
        out_specs=[anywhere] * len(pieces),
        out_shape=[jax.ShapeDtypeStruct(piece.shape, BF16) for piece in pieces],
        scratch_shapes=[
            pltpu.VMEM((m, d), BF16),
            pltpu.VMEM((4, d, f), BF16),
            pltpu.VMEM((2 * f, d), BF16),
            pltpu.VMEM((m, 2 * f), BF16),
            pltpu.VMEM((m, d), BF16),
            pltpu.SemaphoreType.DMA((copies,)),
        ],
        compiler_params=pltpu.CompilerParams(vmem_limit_bytes=(20 if m <= 256 else 24) * 2**20),
        cost_estimate=pl.CostEstimate(
            flops=12 * m * d * f, bytes_accessed=12 * d * f + 6 * m * d, transcendentals=2 * m * f
        ),
    )(*pieces, *gates, *lins, *downs)


def mixer(turn, conv_value, conv_gate, conv_kernel, norm_gain, mixer_proj):
    t = turn[:1].reshape(1, 1, 1)
    first_core, first_x = (t & 1) == 0, (t[0] >> 1) == 0
    gated = lambda value, gate: (value.astype(F32) * jax.nn.sigmoid(gate.astype(F32))).astype(BF16)
    glu = gated(conv_value, conv_gate)
    reach = conv_kernel.shape[0] - 1
    length = glu.shape[0]
    rim = passed_along(gated(conv_value[length - reach :], conv_gate[length - reach :]), "ep", 1)
    padded = jnp.concatenate([rim, glu], axis=0).astype(F32)
    conv = jnp.zeros(glu.shape, F32)
    for tap in range(reach + 1):
        conv = conv + conv_kernel[tap][None, :] * padded[tap : tap + length]
    sums = jnp.stack([jnp.sum(conv, axis=1), jnp.sum(conv * conv, axis=1)])
    sums = sums + tp_swap(sums, 1)
    sums = sums + tp_swap(sums, 2)
    channels = conv.shape[1] * lax.axis_size("tp")
    mean = (sums[0] / channels)[:, None]
    var = (sums[1] / channels)[:, None] - mean * mean
    act = jax.nn.silu((conv - mean) * lax.rsqrt(var + EPS) * norm_gain).astype(BF16)
    rows = length // 4
    act = act.reshape(2, 2, rows, -1)
    mine = jnp.where(first_core, act[:, 0], act[:, 1])
    other = tp_swap(jnp.where(first_core, act[:, 1], act[:, 0]), 1)
    proj_other = tp_swap(mixer_proj, 1)
    flat = lambda a: a.reshape(2 * rows, -1)
    part = dot(flat(mine), mixer_proj) + dot(flat(other), proj_other)
    part = part.reshape(2, rows, -1).astype(BF16)
    away = tp_swap(jnp.where(first_x, part[1], part[0]), 2)
    kept = jnp.where(first_x, part[0], part[1])
    return (kept.astype(F32) + away.astype(F32)).astype(BF16)


def experts_layer(turn, moe_in, route_ids, route_logits, moe_gain, expert_gate, expert_lin, expert_down):
    tp_size = lax.axis_size("tp")
    experts = lax.axis_size("ep")
    rows = moe_in.shape[0] // tp_size
    capacity = max(2, 2 * rows * route_ids.shape[1] // experts)
    few = few_experts(experts)
    close = experts // 2 if few else 0
    layout = {"turned": few, "far": close}
    layout["outs"] = [[(0, place, 1), (1, place, 1)] for place in range(close)]
    layout["outs"] += [[(0, place, 1)] for place in range(close, experts)] if few else [[(0, 0, experts)]]
    slots, slots_far, *packs = pack_tokens(turn, moe_in, route_ids, moe_gain, capacity, layout)
    gates = (expert_gate[0], tp_swap(expert_gate[0], 1))
    lins = (expert_lin[0], tp_swap(expert_lin[0], 1))
    downs = (expert_down[0], tp_swap(expert_down[0], 1))

    def through_expert(chunk):
        return expert_rows(chunk, gates, lins, downs)

    def exchanged_through_expert(rows):
        kept, sent = through_expert([rows, tp_swap(rows, 2)])
        away = tp_swap(sent, 2)
        return (kept.astype(F32) + away.astype(F32)).astype(BF16)

    if few:
        rows_of = [ep_swap(pack, p) if p else pack for p, pack in enumerate(packs)]
        outs = []
        for p in range(0, close, 2):
            outs += through_expert(rows_of[p : p + 2])
        outs += [exchanged_through_expert(rows_of[p]) for p in range(close, experts)]
        pieces = [ep_swap(out, p) if p else out for p, out in enumerate(outs)]
        dense = merge_rows(
            slots_far, route_logits, turn[1:2], pieces[:close], [(capacity, capacity)] * close
        )
        extra = (tp_swap(dense, 2),)
        parts = [(0, capacity)] * experts
    else:
        exchange = lambda a: lax.all_to_all(
            a.reshape(experts, capacity, -1), "ep", split_axis=0, concat_axis=0, tiled=True
        ).reshape(a.shape)
        pieces = [exchange(exchanged_through_expert(exchange(packs[0])))]
        extra, parts = (), [(0, experts * capacity)]
    return merge_rows(slots, route_logits, turn[:1], pieces, parts, extra)


def shards(
    conv_value,
    conv_gate,
    conv_kernel,
    norm_gain,
    mixer_proj,
    moe_in,
    route_ids,
    route_logits,
    moe_gain,
    expert_gate,
    expert_lin,
    expert_down,
):
    t = lax.axis_index("tp")
    turn = lax.optimization_barrier(jnp.stack([t, t ^ 2, lax.axis_index("ep")]))
    mixer_out = mixer(turn, conv_value, conv_gate, conv_kernel, norm_gain, mixer_proj)
    moe_out = experts_layer(
        turn, moe_in, route_ids, route_logits, moe_gain, expert_gate, expert_lin, expert_down
    )
    return (mixer_out, moe_out)


def solution(mesh):
    placed = (
        P("ep", "tp"),
        P("ep", "tp"),
        P(None, "tp"),
        P("tp"),
        P("tp", None),
        P("ep", None),
        P("ep", None),
        P("ep", None),
        P(),
        P("ep", None, "tp"),
        P("ep", None, "tp"),
        P("ep", "tp", None),
    )
    return jax.shard_map(
        shards,
        mesh=mesh,
        in_specs=placed,
        out_specs=(P(("ep", "tp"), None), P(("ep", "tp"), None)),
        check_vma=False,
    )
```
